32 devices in a mesh: dp: 4 (over y, x), kv: 4 (over z), tp: 2 (over core).
Axes of the slice: x: 2, y: 2, z: 4, core: 2. Of those that a mesh axis runs over, the one named last changes fastest.
Arguments:
- tokens: bfloat16 [32, 2048], P('dp', 'kv'), may hold values from -6 to 6
- pre_gain: float32 [2048], P('kv'), may hold values from 0.1 to 1.9
- query_weight: bfloat16 [2048, 1024], P('kv', 'tp'), may hold values from -0.125 to 0.125
- key_weight: bfloat16 [2048, 1024], P('kv', 'tp'), may hold values from -0.125 to 0.125
- value_weight: bfloat16 [2048, 1024], P('kv', 'tp'), may hold values from -0.125 to 0.125
- outgate_weight: bfloat16 [2048, 1024], P('kv', 'tp'), may hold values from -0.125 to 0.125
- input_gate_weight: bfloat16 [2048, 4], replicated, may hold values from -0.125 to 0.125
- forget_gate_weight: bfloat16 [2048, 4], replicated, may hold values from -0.125 to 0.125
- cache_keys: bfloat16 [32, 64, 1024], P(('dp', 'kv'), None, 'tp'), may hold values from -6 to 6
- cache_values: bfloat16 [32, 64, 1024], P(('dp', 'kv'), None, 'tp'), may hold values from -6 to 6
- cache_input: float32 [32, 64, 4], P(('dp', 'kv'), None, 'tp'), may hold values from -6 to 250
- cache_forget: float32 [32, 64, 4], P(('dp', 'kv'), None, 'tp'), may hold values from -0.7 to 0
- lengths: int32 [32], P(('dp', 'kv')), may hold values from 1 to 64, 819 in all
- state_matrix: float32 [32, 4, 256, 256], P(('dp', 'kv'), 'tp'), may hold values from -6 to 6
- state_norm: float32 [32, 4, 256], P(('dp', 'kv'), 'tp'), may hold values from -6 to 6
- state_max: float32 [32, 4], P(('dp', 'kv'), 'tp'), may hold values from -4 to 253
- head_gain: float32 [1024], P('tp'), may hold values from 0.1 to 1.9
- out_weight: bfloat16 [1024, 2048], P('tp', 'kv'), may hold values from -0.375 to 0.375
- mixer_gain: float32 [2048], replicated, may hold values from 0.1 to 1.9
- gate_weight: bfloat16 [2048, 5632], P(None, ('kv', 'tp')), may hold values from -0.125 to 0.125
- up_weight: bfloat16 [2048, 5632], P(None, ('kv', 'tp')), may hold values from -0.125 to 0.125
- down_weight: bfloat16 [5632, 2048], P(('kv', 'tp')), may hold values from -0.21875 to 0.21875
Outputs:
- layer_out: bfloat16 [32, 2048], P('dp', ('kv', 'tp'))
The draws below stay inside these ranges and needn't reach their ends.
Inputs may be any that keep to these rules, and one draw needn't show every extreme that they name: `lengths`: positions from a sequence's length on take no part.
All inputs are finite; a program needn't handle non-finite values. No bound on the sum of `lengths` on one device may be relied on, other than what follows from the above.
Results may differ from the reference program's by a relative error of at most 0.018.
Values may be sent and summed in bfloat16 or wider, within the bound.
A program may use at most 64 MiB of HBM per device.

```python
import math
import jax
import jax.numpy as jnp
import numpy as np
from jax import lax

D = 2048
MEMORY_HEADS = 4
HEAD_DIM = 256
FF = 5632
FOLD_SPAN = 64
HW = 1024
SEQUENCE_TOTAL = 32
N_TP = 2


def draw_cache_input(key, part):
    noise = jnp.clip(jax.random.normal(jax.random.fold_in(key, 11), (SEQUENCE_TOTAL, FOLD_SPAN, MEMORY_HEADS), jnp.float32), -6.0, 6.0)
    return noise


def draw_state_max(key, part):
    noise = jnp.clip(jax.random.normal(jax.random.fold_in(key, 13), (SEQUENCE_TOTAL, MEMORY_HEADS), jnp.float32), -4.0, 4.0)
    return noise


def draw_cache_forget(key, part):
    divided_random_keys = jax.random.split(jax.random.fold_in(key, 17), 6)
    fast_share = 0.5
    fast = jax.random.bernoulli(divided_random_keys[0], fast_share, (SEQUENCE_TOTAL, MEMORY_HEADS))
    fast_rate = jax.random.uniform(divided_random_keys[1], (SEQUENCE_TOTAL, MEMORY_HEADS), jnp.float32, math.log(10.0) / 50.0, math.log(10.0) / 30.0)
    slow_rate = jax.random.uniform(divided_random_keys[2], (SEQUENCE_TOTAL, MEMORY_HEADS), jnp.float32, 0.1, 0.8) * (math.log(10.0) / FOLD_SPAN)
    rate = jnp.where(fast, fast_rate, slow_rate)
    jitter = jax.random.uniform(divided_random_keys[3], (SEQUENCE_TOTAL, FOLD_SPAN, MEMORY_HEADS), jnp.float32, 0.5, 1.5)
    retain_logarithm = -rate[:, None, :] * jitter
    sudden_spike = jax.random.bernoulli(divided_random_keys[4], 3.0 / FOLD_SPAN, (SEQUENCE_TOTAL, FOLD_SPAN, MEMORY_HEADS))
    discarded_entries = jnp.log(jax.random.uniform(divided_random_keys[5], (SEQUENCE_TOTAL, FOLD_SPAN, MEMORY_HEADS), jnp.float32, 0.5, 0.8))
    return jnp.where(sudden_spike, discarded_entries, retain_logarithm)


def spiked(values, key, source, target, blocks, factor):
    owner, partner = [(jnp.arange(values.shape[position]) // (values.shape[position] // blocks)).reshape([-1 if axis == position else 1 for axis in range(values.ndim)]) for position in (source, target)]
    chosen = jax.random.permutation(key, blocks)[partner]
    strong = (owner == chosen) | (owner == (partner + blocks // 2) % blocks)
    return jnp.where(strong, factor * values, values)


def block_levels(stream_key, shape, cuts, low, largest):
    level = 1.0
    for axis_at, blocks in cuts:
        draws = jax.random.uniform(jax.random.fold_in(jax.random.fold_in(stream_key, 6), axis_at), (blocks,), jnp.float32, low / len(cuts), largest / len(cuts))
        level = level * jnp.repeat(jnp.exp(draws), shape[axis_at] // blocks).reshape((-1,) + (1,) * (len(shape) - 1 - axis_at))
    return level


def split_up(number_of, total, limit, slope):
    weights = [(1 << 20) // math.isqrt(grade ** slope) + 1 for grade in range(2, number_of + 1)]
    surplus, counts = total - limit - (number_of - 1), [1] * (number_of - 1)
    while surplus > 0:
        candidates = [i for i in range(number_of - 1) if counts[i] < limit]
        whole, remaining = sum([weights[i] for i in candidates]), surplus
        for i in candidates:
            addition = min(limit - counts[i], max(1, remaining * weights[i] // whole), surplus)
            counts[i] = counts[i] + addition
            surplus = surplus - addition
    return np.array([limit] + counts)


def ragged_sizes(own_key, amount, total, most, slope):
    if amount == 2:
        one = jax.random.randint(own_key, (), max(1, total - most), min(most, total - 1) + 1)
        return jnp.stack([one, total - one])
    sizes = jnp.asarray(split_up(amount, total, most, slope), jnp.int32)
    twos = (amount - 1) // 2
    donor, sink = sizes[1:1 + 2 * twos:2], sizes[2:2 + 2 * twos:2]
    room = jnp.minimum(donor - 1, most - sink)
    moved = jax.random.randint(jax.random.fold_in(own_key, 1), (twos,), 0, 1 << 20) % (room + 1)
    sizes = sizes.at[1:1 + 2 * twos:2].set(donor - moved).at[2:2 + 2 * twos:2].set(sink + moved)
    return sizes[jax.random.permutation(jax.random.fold_in(own_key, 2), amount)]


def gaussian(rng, extent, scale, reach, cuts=(), kind=jnp.bfloat16):
    level = block_levels(rng, extent, cuts, -0.22, 0.18) if cuts else 1.0
    result = jax.random.normal(rng, extent, jnp.float32) * scale * level
    return jnp.minimum(jnp.maximum(result, -reach), reach).astype(kind)


def gaussian_with(key, extent, spread, reach, cuts, heavy, held_as=jnp.bfloat16):
    array = spread * jax.random.normal(key, extent, jnp.float32)
    if cuts:
        array = array * block_levels(key, extent, cuts, -0.22, 0.18)
    return jnp.clip(spiked(array, jax.random.fold_in(key, 3), *heavy), -reach, reach).astype(held_as)


def setup_inputs(seed: int = 0) -> dict:
    key_of = jax.random.split(jax.random.key(seed), 23)
    return {
        "tokens": gaussian_with(key_of[0], (SEQUENCE_TOTAL, D), 1.0, 6.0, ((0, 4), (1, 4)), (1, 0, 4, 2.0)),
        "pre_gain": jnp.clip(1.0 + 0.18 * jax.random.normal(key_of[1], (D,), jnp.float32), 0.1, 1.9),
        "query_weight": gaussian(key_of[2], (D, HW), D ** -0.5, 0.125, ((0, 4), (1, 2))),
        "key_weight": gaussian(key_of[3], (D, HW), D ** -0.5, 0.125, ((0, 4), (1, 2))),
        "value_weight": gaussian(key_of[4], (D, HW), D ** -0.5, 0.125, ((0, 4), (1, 2))),
        "outgate_weight": gaussian(key_of[5], (D, HW), D ** -0.5, 0.125, ((0, 4), (1, 2))),
        "input_gate_weight": gaussian(key_of[6], (D, MEMORY_HEADS), D ** -0.5, 0.125),
        "forget_gate_weight": gaussian(key_of[7], (D, MEMORY_HEADS), D ** -0.5, 0.125),
        "cache_keys": gaussian(key_of[8], (SEQUENCE_TOTAL, FOLD_SPAN, HW), 1.0, 6.0, ((0, 16), (2, 2))),
        "cache_values": gaussian(key_of[9], (SEQUENCE_TOTAL, FOLD_SPAN, HW), 1.0, 6.0, ((0, 16), (2, 2))),
        "cache_input": draw_cache_input(jax.random.fold_in(key_of[22], 71), 0),
        "cache_forget": draw_cache_forget(jax.random.fold_in(key_of[22], 71), 0),
        "lengths": ragged_sizes(key_of[12], SEQUENCE_TOTAL, SEQUENCE_TOTAL * FOLD_SPAN * 2 // 5, FOLD_SPAN, 2).astype(jnp.int32),
        "state_matrix": gaussian(key_of[13], (SEQUENCE_TOTAL, MEMORY_HEADS, HEAD_DIM, HEAD_DIM), 1.0, 6.0, ((0, 16), (1, 2)), jnp.float32),
        "state_norm": gaussian(key_of[14], (SEQUENCE_TOTAL, MEMORY_HEADS, HEAD_DIM), 1.0, 6.0, ((0, 16), (1, 2)), jnp.float32),
        "state_max": draw_state_max(jax.random.fold_in(key_of[22], 71), 0),
        "head_gain": jnp.clip(1.0 + 0.18 * jax.random.normal(key_of[16], (HW,), jnp.float32), 0.1, 1.9),
        "out_weight": gaussian(key_of[17], (HW, D), (HW // 4) ** -0.5, 0.375, ((0, 2), (1, 4))),
        "mixer_gain": jnp.clip(1.0 + 0.18 * jax.random.normal(key_of[18], (D,), jnp.float32), 0.1, 1.9),
        "gate_weight": gaussian(key_of[19], (D, FF), D ** -0.5, 0.125, ((1, 8),)),
        "up_weight": gaussian(key_of[20], (D, FF), D ** -0.5, 0.125, ((1, 8),)),
        "down_weight": gaussian_with(key_of[21], (FF, D), (FF // 4) ** -0.5, 0.21875, ((0, 8),), (0, 1, 8, 2.0)),
    }


EPS = 1e-06

def reference(tokens, pre_gain, query_weight, key_weight, value_weight, outgate_weight, input_gate_weight, forget_gate_weight, cache_keys, cache_values, cache_input, cache_forget, lengths, state_matrix, state_norm, state_max, head_gain, out_weight, mixer_gain, gate_weight, up_weight, down_weight):
    token_values = tokens.astype(jnp.float32)
    scale_first = lax.rsqrt(lax.optimization_barrier(jnp.mean(token_values * token_values, axis=1)) + EPS)[:, None]
    normed_first = (token_values * pre_gain[None, :]).astype(jnp.bfloat16)

    def project(weight):
        return scale_first * jnp.dot(normed_first, weight, preferred_element_type=jnp.float32)
    query = project(query_weight).astype(jnp.bfloat16)
    keys_new = project(key_weight).astype(jnp.bfloat16)
    values_new = project(value_weight).astype(jnp.bfloat16)
    outgate = project(outgate_weight).astype(jnp.bfloat16)
    in_gate = project(input_gate_weight)
    forget_new = jax.nn.log_sigmoid(project(forget_gate_weight))
    seq_count = tokens.shape[0]
    query_heads = query.astype(jnp.float32).reshape(seq_count, MEMORY_HEADS, HEAD_DIM) * HEAD_DIM ** (-0.5)
    key_heads = keys_new.astype(jnp.float32).reshape(seq_count, MEMORY_HEADS, HEAD_DIM)
    value_heads = values_new.astype(jnp.float32).reshape(seq_count, MEMORY_HEADS, HEAD_DIM)
    cached_keys = cache_keys.astype(jnp.float32).reshape(seq_count, FOLD_SPAN, MEMORY_HEADS, HEAD_DIM)
    cached_values = cache_values.astype(jnp.float32).reshape(seq_count, FOLD_SPAN, MEMORY_HEADS, HEAD_DIM)
    live_mask = (jnp.arange(FOLD_SPAN, dtype=jnp.int32)[None, :] < lengths[:, None])[:, :, None]
    forget_live = jnp.where(live_mask, cache_forget, jnp.float32(0.0))
    running = jnp.cumsum(forget_live, axis=1)
    total_log = running[:, -1, :] + forget_new
    weight_log = jnp.where(live_mask, total_log[:, None, :] - running + cache_input, -jnp.inf)
    state_log = total_log + state_max
    peak_log = jnp.maximum(jnp.maximum(state_log, in_gate), lax.optimization_barrier(jnp.max(weight_log, axis=1)))
    key_dots = jnp.einsum('bhd,blhd->blh', query_heads, cached_keys)
    block_scores = jnp.exp(weight_log - peak_log[:, None, :]) * key_dots
    self_score = jnp.exp(in_gate - peak_log) * lax.optimization_barrier(jnp.sum(query_heads * key_heads, axis=2))
    carried = jnp.exp(state_log - peak_log)
    block_weights = lax.optimization_barrier(block_scores.astype(jnp.bfloat16)).astype(jnp.float32)
    memory_read = jnp.einsum('bhvd,bhd->bhv', state_matrix, query_heads, precision=lax.Precision.HIGHEST)
    norm_read = jnp.einsum('bhd,bhd->bh', state_norm, query_heads, precision=lax.Precision.HIGHEST)
    numerator = carried[:, :, None] * memory_read + jnp.einsum('blh,blhd->bhd', block_weights, cached_values) + self_score[:, :, None] * value_heads
    denominator = carried * norm_read + lax.optimization_barrier(jnp.sum(block_scores, axis=1)) + self_score
    hidden = numerator / jnp.maximum(jnp.abs(denominator), 1.0)[:, :, None]
    mixed_heads = (hidden.reshape(seq_count, HW) * head_gain[None, :] * jax.nn.sigmoid(outgate.astype(jnp.float32))).astype(jnp.bfloat16)
    half_width = HW // N_TP
    mix_sum = jnp.zeros((seq_count, D), jnp.float32)
    for half_part in range(N_TP):
        piece_sum = jnp.dot(mixed_heads[:, half_part * half_width:(half_part + 1) * half_width], out_weight[half_part * half_width:(half_part + 1) * half_width], preferred_element_type=jnp.float32)
        mix_sum = mix_sum + lax.optimization_barrier(piece_sum.astype(jnp.bfloat16)).astype(jnp.float32)
    residual = (token_values + mix_sum).astype(jnp.bfloat16)
    residual_values = residual.astype(jnp.float32)
    scale_mid = lax.rsqrt(lax.optimization_barrier(jnp.mean(residual_values * residual_values, axis=1)) + EPS)[:, None]
    normed_mid = (residual_values * mixer_gain[None, :]).astype(jnp.bfloat16)
    gate_values = scale_mid * jnp.dot(normed_mid, gate_weight, preferred_element_type=jnp.float32)
    up_values = scale_mid * jnp.dot(normed_mid, up_weight, preferred_element_type=jnp.float32)
    hidden_units = (jax.nn.silu(gate_values) * up_values).astype(jnp.bfloat16)
    return (residual_values + jnp.dot(hidden_units, down_weight, preferred_element_type=jnp.float32)).astype(jnp.bfloat16)
```

```python
import functools

import jax
import jax.numpy as jnp
from jax import lax
from jax.experimental import pallas as pl
from jax.experimental.pallas import tpu as pltpu
from jax.sharding import PartitionSpec as P

EPS = 1e-06


def per_device(
    tokens,
    pre_gain,
    query_weight,
    key_weight,
    value_weight,
    outgate_weight,
    input_gate_weight,
    forget_gate_weight,
    cache_keys,
    cache_values,
    cache_input,
    cache_forget,
    lengths,
    state_matrix,
    state_norm,
    state_max,
    head_gain,
    out_weight,
    mixer_gain,
    gate_weight,
    up_weight,
    down_weight,
):
    col_width = tokens.shape[1]
    own_seqs = cache_keys.shape[0]
    block_len = cache_keys.shape[1]
    head_count = state_max.shape[1]
    head_size = state_norm.shape[2]
    shard_index = lax.axis_index("kv")
    half_index = lax.axis_index("tp")
    kv_count = lax.axis_size("kv")
    model_width = col_width * kv_count
    token_values = tokens.astype(jnp.float32)
    squares = jnp.sum(token_values * token_values, axis=1)
    normed = (token_values * pre_gain[None, :]).astype(jnp.bfloat16)
    corner = (shard_index * col_width, half_index * head_count)
    gate_pair = jnp.concatenate(
        [
            lax.dynamic_slice(input_gate_weight, corner, (col_width, head_count)),
            lax.dynamic_slice(forget_gate_weight, corner, (col_width, head_count)),
        ],
        axis=1,
    )

    def product(weight):
        return jnp.dot(normed, weight, preferred_element_type=jnp.float32)

    query_term = product(query_weight)
    key_term = product(key_weight)
    value_term = product(value_weight)
    outgate_term = product(outgate_weight)
    gate_term = product(gate_pair)
    square_totals = lax.psum(squares, "kv")
    query_sum, key_sum, value_sum, outgate_sum, gate_sum = (
        lax.psum_scatter(query_term, "kv", scatter_dimension=0, tiled=True),
        lax.psum_scatter(key_term, "kv", scatter_dimension=0, tiled=True),
        lax.psum_scatter(value_term, "kv", scatter_dimension=0, tiled=True),
        lax.psum_scatter(outgate_term, "kv", scatter_dimension=0, tiled=True),
        lax.psum_scatter(gate_term, "kv", scatter_dimension=0, tiled=True),
    )
    own_squares = lax.dynamic_slice_in_dim(square_totals, shard_index * own_seqs, own_seqs, 0)
    scale_first = lax.rsqrt(own_squares / model_width + EPS)[:, None]
    query = (scale_first * query_sum).astype(jnp.bfloat16)
    keys_new = (scale_first * key_sum).astype(jnp.bfloat16)
    values_new = (scale_first * value_sum).astype(jnp.bfloat16)
    outgate = (scale_first * outgate_sum).astype(jnp.bfloat16)
    gate_values = scale_first * gate_sum
    in_gate = gate_values[:, :head_count]
    forget_new = jax.nn.log_sigmoid(gate_values[:, head_count:])
    query_heads = query.reshape(own_seqs, head_count, head_size)
    key_heads = keys_new.reshape(own_seqs, head_count, head_size)
    value_heads = values_new.reshape(own_seqs, head_count, head_size)
    cached_keys = cache_keys.reshape(own_seqs, block_len, head_count, head_size)
    cached_values = cache_values.reshape(own_seqs, block_len, head_count, head_size)
    inv_root = head_size ** (-0.5)
    live_mask = (lax.broadcasted_iota(jnp.int32, (own_seqs, block_len), 1) < lengths[:, None])[
        :, :, None
    ]
    forget_live = jnp.where(live_mask, cache_forget, jnp.float32(0.0))
    running = jnp.cumsum(forget_live, axis=1)
    total_log = running[:, -1, :] + forget_new
    weight_log = jnp.where(live_mask, total_log[:, None, :] - running + cache_input, -jnp.inf)
    state_log = total_log + state_max
    peak_log = jnp.maximum(jnp.maximum(state_log, in_gate), jnp.max(weight_log, axis=1))
    key_dots = (
        jnp.einsum("shd,slhd->slh", query_heads, cached_keys, preferred_element_type=jnp.float32)
        * inv_root
    )
    block_scores = jnp.exp(weight_log - peak_log[:, None, :]) * key_dots
    query_scaled = query_heads.astype(jnp.float32) * inv_root
    self_score = jnp.exp(in_gate - peak_log) * jnp.sum(
        query_scaled * key_heads.astype(jnp.float32), axis=2
    )
    carried = jnp.exp(state_log - peak_log)
    block_weights = block_scores.astype(jnp.bfloat16)
    memory_read = jnp.einsum(
        "shvd,shd->shv", state_matrix, query_scaled, precision=lax.Precision.HIGHEST
    )
    norm_read = jnp.einsum("shd,shd->sh", state_norm, query_scaled, precision=lax.Precision.HIGHEST)
    numerator = (
        carried[:, :, None] * memory_read
        + jnp.einsum(
            "slh,slhd->shd", block_weights, cached_values, preferred_element_type=jnp.float32
        )
        + self_score[:, :, None] * value_heads.astype(jnp.float32)
    )
    denominator = carried * norm_read + jnp.sum(block_scores, axis=1) + self_score
    hidden = numerator / jnp.maximum(jnp.abs(denominator), 1.0)[:, :, None]
    mixed_heads = (
        hidden.reshape(own_seqs, head_count * head_size)
        * head_gain[None, :]
        * jax.nn.sigmoid(outgate.astype(jnp.float32))
    ).astype(jnp.bfloat16)
    mix_terms = jnp.dot(
        lax.all_gather(mixed_heads, "kv", axis=0, tiled=True),
        out_weight,
        preferred_element_type=jnp.float32,
    )
    mix_sum = lax.psum_scatter(
        mix_terms.astype(jnp.bfloat16), "tp", scatter_dimension=1, tiled=True
    ).astype(jnp.float32)
    narrow = mix_sum.shape[1]
    residual = (
        lax.dynamic_slice_in_dim(token_values, half_index * narrow, narrow, 1) + mix_sum
    ).astype(jnp.bfloat16)
    piece_wide = lax.all_gather(residual, ("kv", "tp"), axis=1, tiled=True).astype(jnp.float32)
    normed_piece = (piece_wide * mixer_gain[None, :]).astype(jnp.bfloat16)
    gate_acc = jnp.dot(normed_piece, gate_weight, preferred_element_type=jnp.float32)
    up_acc = jnp.dot(normed_piece, up_weight, preferred_element_type=jnp.float32)
    sum_squares = jnp.sum(piece_wide * piece_wide, axis=1)
    gate_acc, up_acc, sum_squares = (gate_acc, up_acc, sum_squares)
    scale_mid = lax.rsqrt(sum_squares / model_width + EPS)[:, None]
    hidden_units = (jax.nn.silu(scale_mid * gate_acc) * (scale_mid * up_acc)).astype(jnp.bfloat16)
    summed = lax.psum_scatter(
        lax.dot_general(
            down_weight, hidden_units, (((0,), (1,)), ((), ())), preferred_element_type=jnp.float32
        ),
        ("kv", "tp"),
        scatter_dimension=0,
        tiled=True,
    )
    mixer_out = summed.T
    return (residual.astype(jnp.float32) + mixer_out).astype(jnp.bfloat16)


def cell_kernel(
    kv_count,
    tp_count,
    tokens,
    pre_gain,
    query_weight,
    key_weight,
    value_weight,
    outgate_weight,
    input_gate_weight,
    forget_gate_weight,
    cache_keys,
    cache_values,
    cache_input,
    cache_forget,
    lengths,
    state_matrix,
    state_norm,
    state_max,
    head_gain,
    out_weight,
    mixer_gain,
    gate_weight,
    up_weight,
    down_weight,
    out,
    tok_v,
    pg_v,
    proj_v,
    igw_v,
    fgw_v,
    ck_v,
    cv_v,
    ci_v,
    cf_v,
    len_v,
    sm_v,
    sn_v,
    sx_v,
    hg_v,
    outw_v,
    mg_v,
    gw_v,
    uw_v,
    dw_v,
    hi_v,
    lo_v,
    proj_send,
    proj_recv,
    tok_recv,
    mixed_all,
    half_send,
    half_recv,
    down_send,
    down_recv,
    local_sem,
    proj_ssem,
    proj_rsem,
    tok_ssem,
    tok_rsem,
    mixed_ssem,
    mixed_rsem,
    half_ssem,
    half_rsem,
    down_ssem,
    down_rsem,
):
    f32, bf16 = jnp.float32, jnp.bfloat16
    me = lax.axis_index("kv")
    core = lax.axis_index("tp")
    rows, width = tok_v.shape
    own_seqs, block_len = ck_v.shape[0], ck_v.shape[1]
    head_count, head_size = sn_v.shape[1], sn_v.shape[2]
    own_width = head_count * head_size
    model_width = width * kv_count
    narrow = out.shape[1]
    peers = [(dk, dt) for dk in range(kv_count) for dt in range(tp_count) if dk or dt]
    far_first = sorted(range(len(peers)), key=lambda i: -min(peers[i][0], kv_count - peers[i][0]))
    near_first = far_first[::-1]
    kv_far = sorted(range(1, kv_count), key=lambda d: -min(d, kv_count - d))

    def peer(dk, dt):
        return {"kv": lax.rem(me + dk, kv_count), "tp": lax.rem(core + dt, tp_count)}

    sources = (
        (tokens, tok_v),
        (pre_gain, pg_v),
        (query_weight, proj_v.at[0]),
        (key_weight, proj_v.at[1]),
        (value_weight, proj_v.at[2]),
        (outgate_weight, proj_v.at[3]),
        (input_gate_weight.at[:, pl.ds(pl.multiple_of(me * width, 128), width)], igw_v),
        (forget_gate_weight.at[:, pl.ds(pl.multiple_of(me * width, 128), width)], fgw_v),
        (cache_forget, cf_v),
        (cache_input, ci_v),
        (lengths, len_v),
        (state_max, sx_v),
        (state_norm, sn_v),
        (head_gain, hg_v),
        (state_matrix, sm_v),
        (cache_keys, ck_v),
        (cache_values, cv_v),
        (out_weight, outw_v),
        (mixer_gain, mg_v),
        (gate_weight, gw_v),
        (up_weight, uw_v),
        (down_weight, dw_v),
    )
    loads = [
        pltpu.make_async_copy(src, dst, local_sem.at[i]) for i, (src, dst) in enumerate(sources)
    ]
    for load in loads:
        load.start()

    barrier = pltpu.get_barrier_semaphore()
    for dk, dt in peers:
        pl.semaphore_signal(
            barrier, inc=1, device_id=peer(dk, dt), device_id_type=pl.DeviceIdType.MESH
        )

    def remote(src, dst, ssem, rsem, dk, dt):
        return pltpu.make_async_remote_copy(
            src_ref=src,
            dst_ref=dst,
            send_sem=ssem,
            recv_sem=rsem,
            device_id=peer(dk, dt),
            device_id_type=pl.DeviceIdType.MESH,
        )

    for i in range(2):
        loads[i].wait()
    token_values = tok_v[...].astype(f32)
    squares = jnp.sum(token_values * token_values, axis=1, keepdims=True)
    normed = (token_values * pg_v[...]).astype(bf16)
    for i in range(4):
        loads[2 + i].wait()
        term = jnp.dot(normed, proj_v[i], preferred_element_type=f32)
        for r in range(kv_count):
            proj_send[r, own_seqs * i : own_seqs * (i + 1), :own_width] = term[
                own_seqs * r : own_seqs * (r + 1), :
            ]
    loads[6].wait()
    loads[7].wait()
    contract_last = (((1,), (1,)), ((), ()))
    gates = [
        lax.dot_general(normed, ref[...], contract_last, preferred_element_type=f32)
        for ref in (igw_v, fgw_v)
    ]
    lane = lax.broadcasted_iota(jnp.int32, (rows, 128), 1)
    small = jnp.where(lane == 2 * head_count, squares, 0.0)
    for g in range(2):
        for h in range(head_count):
            column = gates[g][:, h : h + 1]
            for t in range(1, tp_count):
                at = t * head_count + h
                column = jnp.where(core == t, gates[g][:, at : at + 1], column)
            small = jnp.where(lane == g * head_count + h, column, small)
    for r in range(kv_count):
        for i in range(4):
            proj_send[r, own_seqs * i : own_seqs * (i + 1), own_width:] = small[
                own_seqs * r : own_seqs * (r + 1), :
            ]

    pl.semaphore_wait(barrier, len(peers))
    proj_copies = {}
    for d in kv_far:
        proj_copies[d] = remote(
            proj_send.at[lax.rem(me + d, kv_count)],
            proj_recv.at[d - 1],
            proj_ssem.at[d - 1],
            proj_rsem.at[d - 1],
            d,
            0,
        )
        proj_copies[d].start()
    tok_copies = {}
    for d in kv_far:
        tok_copies[d] = remote(
            tok_v, tok_recv.at[d - 1], tok_ssem.at[d - 1], tok_rsem.at[d - 1], d, 0
        )
        tok_copies[d].start()

    for i in range(8, 15):
        loads[i].wait()
    for s in range(own_seqs):
        for h in range(head_count):
            whole = sm_v[s, h]
            high = whole.astype(bf16)
            hi_v[s, h] = high
            lo_v[s, h] = (whole - high.astype(f32)).astype(bf16)
    at_row = lax.broadcasted_iota(jnp.int32, (block_len, block_len), 0)
    at_col = lax.broadcasted_iota(jnp.int32, (block_len, block_len), 1)
    position_row = lax.broadcasted_iota(jnp.int32, (1, block_len), 1)
    base_log, base_max, base_total = {}, {}, {}
    for s in range(own_seqs):
        length = len_v[0:1, s : s + 1]
        forget_all = cf_v[s]
        input_all = ci_v[s]
        for h in range(head_count):
            forget_column = jnp.broadcast_to(forget_all[:, h : h + 1], (block_len, block_len))
            input_column = jnp.broadcast_to(input_all[:, h : h + 1], (block_len, block_len))
            counted = (at_row <= at_col) & (at_row < length)
            running = jnp.sum(jnp.where(counted, forget_column, 0.0), axis=0, keepdims=True)
            inputs = jnp.sum(
                jnp.where(at_row == at_col, input_column, 0.0), axis=0, keepdims=True
            )
            total = running[:, block_len - 1 : block_len]
            logs = jnp.where(position_row < length, total - running + inputs, -jnp.inf)
            base_log[s, h] = logs
            base_max[s, h] = jnp.max(logs, axis=1, keepdims=True)
            base_total[s, h] = total
    for i in range(15, 17):
        loads[i].wait()

    summed = proj_send[me]
    for d in range(1, kv_count):
        proj_copies[d].wait_recv()
        summed = summed + proj_recv[d - 1]
    inv_root = head_size ** (-0.5)
    mixed_rows = []
    for s in range(own_seqs):
        tail = summed[s : s + 1, own_width:]
        square = tail[:, 2 * head_count : 2 * head_count + 1]
        scale_first = lax.rsqrt(square / model_width + EPS)
        tail = tail * scale_first
        query, key, value, outgate = (
            (scale_first * summed[own_seqs * i + s : own_seqs * i + s + 1, :own_width])
            .astype(bf16)
            .astype(f32)
            for i in range(4)
        )
        query = query * inv_root
        hidden_parts = []
        for h in range(head_count):
            cols = slice(h * head_size, (h + 1) * head_size)
            in_gate = tail[:, h : h + 1]
            forget_arg = tail[:, head_count + h : head_count + h + 1]
            forget_new = jnp.minimum(forget_arg, 0.0) - jnp.log1p(jnp.exp(-jnp.abs(forget_arg)))
            state_log = base_total[s, h] + forget_new + sx_v[s : s + 1, h : h + 1]
            peak_log = jnp.maximum(
                jnp.maximum(state_log, in_gate), base_max[s, h] + forget_new
            )
            q = query[:, cols]
            q_low = q.astype(bf16)
            dots = lax.dot_general(
                q_low, ck_v[s, :, cols], contract_last, preferred_element_type=f32
            )
            scores = jnp.exp(base_log[s, h] + forget_new - peak_log) * dots
            self_score = jnp.exp(in_gate - peak_log) * jnp.sum(
                q * key[:, cols], axis=1, keepdims=True
            )
            carried = jnp.exp(state_log - peak_log)
            read = lax.dot_general(
                q_low, hi_v[s, h], contract_last, preferred_element_type=f32
            ) + lax.dot_general(q_low, lo_v[s, h], contract_last, preferred_element_type=f32)
            norm_read = jnp.sum(sn_v[s, h : h + 1, :] * q, axis=1, keepdims=True)
            numerator = (
                carried * read
                + jnp.dot(scores.astype(bf16), cv_v[s, :, cols], preferred_element_type=f32)
                + self_score * value[:, cols]
            )
            denominator = (
                carried * norm_read + jnp.sum(scores, axis=1, keepdims=True) + self_score
            )
            hidden = numerator / jnp.maximum(jnp.abs(denominator), 1.0)
            hidden_parts.append(hidden * hg_v[:, cols] * jax.nn.sigmoid(outgate[:, cols]))
        mixed_rows.append(jnp.concatenate(hidden_parts, axis=1))
    for s in range(own_seqs):
        mixed_all[me, s : s + 1, :] = mixed_rows[s].astype(bf16).astype(f32)
    mixed_copies = {}
    for d in kv_far:
        mixed_copies[d] = remote(
            mixed_all.at[me],
            mixed_all.at[me],
            mixed_ssem.at[d - 1],
            mixed_rsem.at[lax.rem(me + 0, kv_count)],
            d,
            0,
        )
        mixed_copies[d].start()
    loads[17].wait()
    for d in range(1, kv_count):
        source = lax.rem(me + kv_count - d, kv_count)
        remote(
            mixed_all.at[source], mixed_all.at[source], mixed_ssem.at[d - 1],
            mixed_rsem.at[source], d, 0,
        ).wait_recv()
    mixed = jnp.concatenate([mixed_all[r] for r in range(kv_count)], axis=0).astype(bf16)
    own_half = jnp.dot(mixed, outw_v[...], preferred_element_type=f32).astype(bf16)
    half_send[...] = own_half
    half_copies = {}
    for i in far_first:
        dk, dt = peers[i]
        half_copies[i] = remote(
            half_send, half_recv.at[i], half_ssem.at[i], half_rsem.at[i], dk, dt
        )
        half_copies[i].start()
    for i in range(18, 21):
        loads[i].wait()
    sum_squares = jnp.zeros((rows, 1), f32)
    gate_acc = jnp.zeros((rows, gw_v.shape[1]), f32)
    up_acc = jnp.zeros((rows, gw_v.shape[1]), f32)
    own_residual = None
    for dk in sorted(range(kv_count), key=lambda d: min(d, kv_count - d)):
        source = lax.rem(me + kv_count - dk, kv_count)
        halves = [own_half.astype(f32)] if dk == 0 else []
        for i, (pk, pt) in enumerate(peers):
            if pk == dk:
                half_copies[i].wait_recv()
                halves.append(half_recv[i].astype(f32))
        if dk:
            tok_copies[dk].wait_recv()
            chunk_tokens = tok_recv[dk - 1].astype(f32)
        else:
            chunk_tokens = token_values
        residual = (chunk_tokens + sum(halves[1:], halves[0])).astype(bf16).astype(f32)
        if dk == 0:
            own_residual = residual
        sum_squares = sum_squares + jnp.sum(residual * residual, axis=1, keepdims=True)
        at = pl.multiple_of(source * width, 128)
        normed_mid = (residual * mg_v[:, pl.ds(at, width)]).astype(bf16)
        gate_acc = gate_acc + jnp.dot(
            normed_mid, gw_v[pl.ds(at, width), :], preferred_element_type=f32
        )
        up_acc = up_acc + jnp.dot(
            normed_mid, uw_v[pl.ds(at, width), :], preferred_element_type=f32
        )
    scale_mid = lax.rsqrt(sum_squares / model_width + EPS)
    hidden_units = (jax.nn.silu(scale_mid * gate_acc) * (scale_mid * up_acc)).astype(bf16)
    loads[21].wait()

    def down_part(dk, dt):
        target = lax.rem(me + dk, kv_count) * tp_count + lax.rem(core + dt, tp_count)
        at = pl.multiple_of(target * narrow, 128)
        return jnp.dot(hidden_units, dw_v[:, pl.ds(at, narrow)], preferred_element_type=f32)

    down_copies = {}
    for i in far_first:
        dk, dt = peers[i]
        down_send[i] = down_part(dk, dt).astype(down_send.dtype)
        down_copies[i] = remote(
            down_send.at[i], down_recv.at[i], down_ssem.at[i], down_rsem.at[i], dk, dt
        )
        down_copies[i].start()
    total_out = own_residual[:, :narrow]
    for t in range(1, tp_count):
        total_out = jnp.where(
            core == t, own_residual[:, t * narrow : (t + 1) * narrow], total_out
        )
    mixer_out = down_part(0, 0)
    for i in near_first:
        down_copies[i].wait_recv()
        mixer_out = mixer_out + down_recv[i].astype(f32)
    out[...] = (total_out + mixer_out).astype(out.dtype)

    for copies in (proj_copies, tok_copies, mixed_copies, half_copies, down_copies):
        for copy in copies.values():
            copy.wait_send()


def fused_device(mesh, *args):
    (tokens, pre_gain, query_weight, _, _, _, input_gate_weight, forget_gate_weight) = args[:8]
    cache_keys, cache_values, cache_input, cache_forget, lengths = args[8:13]
    state_matrix, state_norm, state_max, head_gain, out_weight = args[13:18]
    mixer_gain, gate_weight, up_weight, down_weight = args[18:]
    kv_count, tp_count = mesh.shape["kv"], mesh.shape["tp"]
    f32, bf16 = jnp.float32, jnp.bfloat16
    rows, width = tokens.shape
    own_seqs = cache_keys.shape[0]
    own_width = query_weight.shape[1]
    narrow = width // tp_count
    peer_count = kv_count * tp_count - 1
    given = list(args)
    given[1] = pre_gain[None, :]
    given[6] = input_gate_weight.T
    given[7] = forget_gate_weight.T
    given[12] = lengths[None, :]
    given[16] = head_gain[None, :]
    given[18] = mixer_gain[None, :]

    def held(array):
        return pltpu.VMEM(array.shape, array.dtype)

    gate_heads = input_gate_weight.shape[1]
    dma = pltpu.SemaphoreType.DMA
    scratch = [
        held(tokens),
        held(given[1]),
        pltpu.VMEM((4,) + query_weight.shape, bf16),
        pltpu.VMEM((gate_heads, width), bf16),
        pltpu.VMEM((gate_heads, width), bf16),
        held(cache_keys),
        held(cache_values),
        held(cache_input),
        held(cache_forget),
        held(given[12]),
        held(state_matrix),
        held(state_norm),
        held(state_max),
        held(given[16]),
        held(out_weight),
        held(given[18]),
        held(gate_weight),
        held(up_weight),
        held(down_weight),
        pltpu.VMEM(state_matrix.shape, bf16),
        pltpu.VMEM(state_matrix.shape, bf16),
        pltpu.VMEM((kv_count, 4 * own_seqs, own_width + 128), f32),
        pltpu.VMEM((kv_count - 1, 4 * own_seqs, own_width + 128), f32),
        pltpu.VMEM((kv_count - 1, rows, width), bf16),
        pltpu.VMEM((kv_count, own_seqs, own_width), f32),
        pltpu.VMEM((rows, width), bf16),
        pltpu.VMEM((peer_count, rows, width), bf16),
        pltpu.VMEM((peer_count, rows, narrow), f32),
        pltpu.VMEM((peer_count, rows, narrow), f32),
        dma((len(args),)),
        dma((kv_count - 1,)),
        dma((kv_count - 1,)),
        dma((kv_count - 1,)),
        dma((kv_count - 1,)),
        dma((kv_count - 1,)),
        dma((kv_count,)),
        dma((peer_count,)),
        dma((peer_count,)),
        dma((peer_count,)),
        dma((peer_count,)),
    ]
    return pl.pallas_call(
        functools.partial(cell_kernel, kv_count, tp_count),
        out_shape=jax.ShapeDtypeStruct((rows, narrow), tokens.dtype),
        in_specs=[pl.BlockSpec(memory_space=pl.ANY)] * len(args),
        out_specs=pl.BlockSpec(memory_space=pltpu.VMEM),
        scratch_shapes=scratch,
        compiler_params=pltpu.CompilerParams(
            collective_id=0, has_side_effects=True, vmem_limit_bytes=60 * 1024 * 1024
        ),
    )(*given)


def fits_tiles(mesh, tokens, query_weight, cache_keys, state_norm):
    kv_count, tp_count = mesh.shape["kv"], mesh.shape["tp"]
    return (
        tokens.shape[1] % (kv_count * tp_count * 128) == 0
        and query_weight.shape[1] % (tp_count * 128) == 0
        and state_norm.shape[2] % 128 == 0
        and kv_count > 1
    )


def solution(mesh):
    in_specs = (
        P("dp", "kv"),
        P("kv"),
        P("kv", "tp"),
        P("kv", "tp"),
        P("kv", "tp"),
        P("kv", "tp"),
        P(),
        P(),
        P(("dp", "kv"), None, "tp"),
        P(("dp", "kv"), None, "tp"),
        P(("dp", "kv"), None, "tp"),
        P(("dp", "kv"), None, "tp"),
        P(("dp", "kv")),
        P(("dp", "kv"), "tp", None, None),
        P(("dp", "kv"), "tp", None),
        P(("dp", "kv"), "tp"),
        P("tp"),
        P("tp", "kv"),
        P(),
        P(None, ("kv", "tp")),
        P(None, ("kv", "tp")),
        P(("kv", "tp"), None),
    )
    out_specs = P("dp", ("kv", "tp"))

    def run(*args):
        fused = fits_tiles(mesh, args[0], args[2], args[8], args[14])
        body = functools.partial(fused_device, mesh) if fused else per_device
        return jax.shard_map(
            body, mesh=mesh, in_specs=in_specs, out_specs=out_specs, check_vma=False
        )(*args)

    return run
```

```python
import functools

import jax
import jax.numpy as jnp
from jax import lax
from jax.experimental import pallas as pl
from jax.experimental.pallas import tpu as pltpu
from jax.sharding import PartitionSpec as P

EPS = 1e-06


def per_device(
    tokens,
    pre_gain,
    query_weight,
    key_weight,
    value_weight,
    outgate_weight,
    input_gate_weight,
    forget_gate_weight,
    cache_keys,
    cache_values,
    cache_input,
    cache_forget,
    lengths,
    state_matrix,
    state_norm,
    state_max,
    head_gain,
    out_weight,
    mixer_gain,
    gate_weight,
    up_weight,
    down_weight,
):
    col_width = tokens.shape[1]
    own_seqs = cache_keys.shape[0]
    block_len = cache_keys.shape[1]
    head_count = state_max.shape[1]
    head_size = state_norm.shape[2]
    shard_index = lax.axis_index("kv")
    half_index = lax.axis_index("tp")
    kv_count = lax.axis_size("kv")
    model_width = col_width * kv_count
    token_values = tokens.astype(jnp.float32)
    squares = jnp.sum(token_values * token_values, axis=1)
    normed = (token_values * pre_gain[None, :]).astype(jnp.bfloat16)
    corner = (shard_index * col_width, half_index * head_count)
    gate_pair = jnp.concatenate(
        [
            lax.dynamic_slice(input_gate_weight, corner, (col_width, head_count)),
            lax.dynamic_slice(forget_gate_weight, corner, (col_width, head_count)),
        ],
        axis=1,
    )

    def product(weight):
        return jnp.dot(normed, weight, preferred_element_type=jnp.float32)

    query_term = product(query_weight)
    key_term = product(key_weight)
    value_term = product(value_weight)
    outgate_term = product(outgate_weight)
    gate_term = product(gate_pair)
    square_totals = lax.psum(squares, "kv")
    query_sum, key_sum, value_sum, outgate_sum, gate_sum = (
        lax.psum_scatter(query_term, "kv", scatter_dimension=0, tiled=True),
        lax.psum_scatter(key_term, "kv", scatter_dimension=0, tiled=True),
        lax.psum_scatter(value_term, "kv", scatter_dimension=0, tiled=True),
        lax.psum_scatter(outgate_term, "kv", scatter_dimension=0, tiled=True),
        lax.psum_scatter(gate_term, "kv", scatter_dimension=0, tiled=True),
    )
    own_squares = lax.dynamic_slice_in_dim(square_totals, shard_index * own_seqs, own_seqs, 0)
    scale_first = lax.rsqrt(own_squares / model_width + EPS)[:, None]
    query = (scale_first * query_sum).astype(jnp.bfloat16)
    keys_new = (scale_first * key_sum).astype(jnp.bfloat16)
    values_new = (scale_first * value_sum).astype(jnp.bfloat16)
    outgate = (scale_first * outgate_sum).astype(jnp.bfloat16)
    gate_values = scale_first * gate_sum
    in_gate = gate_values[:, :head_count]
    forget_new = jax.nn.log_sigmoid(gate_values[:, head_count:])
    query_heads = query.reshape(own_seqs, head_count, head_size)
    key_heads = keys_new.reshape(own_seqs, head_count, head_size)
    value_heads = values_new.reshape(own_seqs, head_count, head_size)
    cached_keys = cache_keys.reshape(own_seqs, block_len, head_count, head_size)
    cached_values = cache_values.reshape(own_seqs, block_len, head_count, head_size)
    inv_root = head_size ** (-0.5)
    live_mask = (lax.broadcasted_iota(jnp.int32, (own_seqs, block_len), 1) < lengths[:, None])[
        :, :, None
    ]
    forget_live = jnp.where(live_mask, cache_forget, jnp.float32(0.0))
    running = jnp.cumsum(forget_live, axis=1)
    total_log = running[:, -1, :] + forget_new
    weight_log = jnp.where(live_mask, total_log[:, None, :] - running + cache_input, -jnp.inf)
    state_log = total_log + state_max
    peak_log = jnp.maximum(jnp.maximum(state_log, in_gate), jnp.max(weight_log, axis=1))
    key_dots = (
        jnp.einsum("shd,slhd->slh", query_heads, cached_keys, preferred_element_type=jnp.float32)
        * inv_root
    )
    block_scores = jnp.exp(weight_log - peak_log[:, None, :]) * key_dots
    query_scaled = query_heads.astype(jnp.float32) * inv_root
    self_score = jnp.exp(in_gate - peak_log) * jnp.sum(
        query_scaled * key_heads.astype(jnp.float32), axis=2
    )
    carried = jnp.exp(state_log - peak_log)
    block_weights = block_scores.astype(jnp.bfloat16)
    memory_read = jnp.einsum(
        "shvd,shd->shv", state_matrix, query_scaled, precision=lax.Precision.HIGHEST
    )
    norm_read = jnp.einsum("shd,shd->sh", state_norm, query_scaled, precision=lax.Precision.HIGHEST)
    numerator = (
        carried[:, :, None] * memory_read
        + jnp.einsum(
            "slh,slhd->shd", block_weights, cached_values, preferred_element_type=jnp.float32
        )
        + self_score[:, :, None] * value_heads.astype(jnp.float32)
    )
    denominator = carried * norm_read + jnp.sum(block_scores, axis=1) + self_score
    hidden = numerator / jnp.maximum(jnp.abs(denominator), 1.0)[:, :, None]
    mixed_heads = (
        hidden.reshape(own_seqs, head_count * head_size)
        * head_gain[None, :]
        * jax.nn.sigmoid(outgate.astype(jnp.float32))
    ).astype(jnp.bfloat16)
    mix_terms = jnp.dot(
        lax.all_gather(mixed_heads, "kv", axis=0, tiled=True),
        out_weight,
        preferred_element_type=jnp.float32,
    )
    mix_sum = lax.psum_scatter(
        mix_terms.astype(jnp.bfloat16), "tp", scatter_dimension=1, tiled=True
    ).astype(jnp.float32)
    narrow = mix_sum.shape[1]
    residual = (
        lax.dynamic_slice_in_dim(token_values, half_index * narrow, narrow, 1) + mix_sum
    ).astype(jnp.bfloat16)
    piece_wide = lax.all_gather(residual, ("kv", "tp"), axis=1, tiled=True).astype(jnp.float32)
    normed_piece = (piece_wide * mixer_gain[None, :]).astype(jnp.bfloat16)
    gate_acc = jnp.dot(normed_piece, gate_weight, preferred_element_type=jnp.float32)
    up_acc = jnp.dot(normed_piece, up_weight, preferred_element_type=jnp.float32)
    sum_squares = jnp.sum(piece_wide * piece_wide, axis=1)
    gate_acc, up_acc, sum_squares = (gate_acc, up_acc, sum_squares)
    scale_mid = lax.rsqrt(sum_squares / model_width + EPS)[:, None]
    hidden_units = (jax.nn.silu(scale_mid * gate_acc) * (scale_mid * up_acc)).astype(jnp.bfloat16)
    summed = lax.psum_scatter(
        lax.dot_general(
            down_weight, hidden_units, (((0,), (1,)), ((), ())), preferred_element_type=jnp.float32
        ),
        ("kv", "tp"),
        scatter_dimension=0,
        tiled=True,
    )
    mixer_out = summed.T
    return (residual.astype(jnp.float32) + mixer_out).astype(jnp.bfloat16)


def cell_kernel(
    kv_count,
    tp_count,
    tokens,
    pre_gain,
    query_weight,
    key_weight,
    value_weight,
    outgate_weight,
    input_gate_weight,
    forget_gate_weight,
    cache_keys,
    cache_values,
    cache_input,
    cache_forget,
    lengths,
    state_matrix,
    state_norm,
    state_max,
    head_gain,
    out_weight,
    mixer_gain,
    gate_weight,
    up_weight,
    down_weight,
    out,
    tok_v,
    pg_v,
    proj_v,
    igw_v,
    fgw_v,
    ck_v,
    cv_v,
    ci_v,
    cf_v,
    len_v,
    sm_v,
    sn_v,
    sx_v,
    hg_v,
    outw_v,
    mg_v,
    gw_v,
    uw_v,
    dw_v,
    hi_v,
    lo_v,
    proj_send,
    proj_recv,
    tok_recv,
    mixed_all,
    half_send,
    half_recv,
    down_send,
    down_recv,
    local_sem,
    proj_ssem,
    proj_rsem,
    tok_ssem,
    tok_rsem,
    mixed_ssem,
    mixed_rsem,
    half_ssem,
    half_rsem,
    down_ssem,
    down_rsem,
):
    f32, bf16 = jnp.float32, jnp.bfloat16
    me = lax.axis_index("kv")
    core = lax.axis_index("tp")
    rows, width = tok_v.shape
    own_seqs, block_len = ck_v.shape[0], ck_v.shape[1]
    head_count, head_size = sn_v.shape[1], sn_v.shape[2]
    own_width = head_count * head_size
    model_width = width * kv_count
    narrow = out.shape[1]
    peers = [(dk, dt) for dk in range(kv_count) for dt in range(tp_count) if dk or dt]
    far_first = sorted(range(len(peers)), key=lambda i: -min(peers[i][0], kv_count - peers[i][0]))
    near_first = far_first[::-1]
    kv_far = sorted(range(1, kv_count), key=lambda d: -min(d, kv_count - d))

    def peer(dk, dt):
        return {"kv": lax.rem(me + dk, kv_count), "tp": lax.rem(core + dt, tp_count)}

    sources = (
        (tokens, tok_v),
        (pre_gain, pg_v),
        (query_weight, proj_v.at[0]),
        (key_weight, proj_v.at[1]),
        (value_weight, proj_v.at[2]),
        (outgate_weight, proj_v.at[3]),
        (input_gate_weight.at[:, pl.ds(pl.multiple_of(me * width, 128), width)], igw_v),
        (forget_gate_weight.at[:, pl.ds(pl.multiple_of(me * width, 128), width)], fgw_v),
        (cache_forget, cf_v),
        (cache_input, ci_v),
        (lengths, len_v),
        (state_max, sx_v),
        (state_norm, sn_v),
        (head_gain, hg_v),
        (state_matrix, sm_v),
        (cache_keys, ck_v),
        (cache_values, cv_v),
        (out_weight, outw_v),
        (mixer_gain, mg_v),
        (gate_weight, gw_v),
        (up_weight, uw_v),
        (down_weight, dw_v),
    )
    loads = [
        pltpu.make_async_copy(src, dst, local_sem.at[i]) for i, (src, dst) in enumerate(sources)
    ]
    for load in loads[:8]:
        load.start()

    barrier = pltpu.get_barrier_semaphore()
    for dk, dt in peers:
        pl.semaphore_signal(
            barrier, inc=1, device_id=peer(dk, dt), device_id_type=pl.DeviceIdType.MESH
        )

    def remote(src, dst, ssem, rsem, dk, dt):
        return pltpu.make_async_remote_copy(
            src_ref=src,
            dst_ref=dst,
            send_sem=ssem,
            recv_sem=rsem,
            device_id=peer(dk, dt),
            device_id_type=pl.DeviceIdType.MESH,
        )

    for i in range(2):
        loads[i].wait()
    token_values = tok_v[...].astype(f32)
    squares = jnp.sum(token_values * token_values, axis=1, keepdims=True)
    normed = (token_values * pg_v[...]).astype(bf16)
    for i in range(4):
        loads[2 + i].wait()
        term = jnp.dot(normed, proj_v[i], preferred_element_type=f32)
        for r in range(kv_count):
            proj_send[r, own_seqs * i : own_seqs * (i + 1), :own_width] = term[
                own_seqs * r : own_seqs * (r + 1), :
            ]
    loads[6].wait()
    loads[7].wait()
    for load in loads[8:]:
        load.start()
    contract_last = (((1,), (1,)), ((), ()))
    gates = [
        lax.dot_general(normed, ref[...], contract_last, preferred_element_type=f32)
        for ref in (igw_v, fgw_v)
    ]
    lane = lax.broadcasted_iota(jnp.int32, (rows, 128), 1)
    small = jnp.where(lane == 2 * head_count, squares, 0.0)
    for g in range(2):
        for h in range(head_count):
            column = gates[g][:, h : h + 1]
            for t in range(1, tp_count):
                at = t * head_count + h
                column = jnp.where(core == t, gates[g][:, at : at + 1], column)
            small = jnp.where(lane == g * head_count + h, column, small)
    for r in range(kv_count):
        for i in range(4):
            proj_send[r, own_seqs * i : own_seqs * (i + 1), own_width:] = small[
                own_seqs * r : own_seqs * (r + 1), :
            ]

    pl.semaphore_wait(barrier, len(peers))
    proj_copies = {}
    for d in kv_far:
        proj_copies[d] = remote(
            proj_send.at[lax.rem(me + d, kv_count)],
            proj_recv.at[d - 1],
            proj_ssem.at[d - 1],
            proj_rsem.at[d - 1],
            d,
            0,
        )
        proj_copies[d].start()
    tok_copies = {}
    for d in kv_far:
        tok_copies[d] = remote(
            tok_v, tok_recv.at[d - 1], tok_ssem.at[d - 1], tok_rsem.at[d - 1], d, 0
        )
        tok_copies[d].start()

    for i in range(8, 15):
        loads[i].wait()
    for s in range(own_seqs):
        for h in range(head_count):
            whole = sm_v[s, h]
            high = whole.astype(bf16)
            hi_v[s, h] = high
            lo_v[s, h] = (whole - high.astype(f32)).astype(bf16)
    at_row = lax.broadcasted_iota(jnp.int32, (block_len, block_len), 0)
    at_col = lax.broadcasted_iota(jnp.int32, (block_len, block_len), 1)
    position_row = lax.broadcasted_iota(jnp.int32, (1, block_len), 1)
    up_to = (at_row <= at_col).astype(f32)
    base_log, base_max, base_total = {}, {}, {}
    for s in range(own_seqs):
        live = position_row < len_v[0:1, s : s + 1]
        running_all = jnp.dot(
            jnp.where(live, cf_v[s], 0.0),
            up_to,
            precision=lax.Precision.HIGHEST,
            preferred_element_type=f32,
        )
        for h in range(head_count):
            running = running_all[h : h + 1, :]
            total = running[:, block_len - 1 : block_len]
            logs = jnp.where(live, total - running + ci_v[s, h : h + 1, :], -jnp.inf)
            base_log[s, h] = logs
            base_max[s, h] = jnp.max(logs, axis=1, keepdims=True)
            base_total[s, h] = total
    for i in range(15, 17):
        loads[i].wait()

    summed = proj_send[me]
    for d in range(1, kv_count):
        proj_copies[d].wait_recv()
        summed = summed + proj_recv[d - 1]
    inv_root = head_size ** (-0.5)
    mixed_rows = []
    for s in range(own_seqs):
        tail = summed[s : s + 1, own_width:]
        square = tail[:, 2 * head_count : 2 * head_count + 1]
        scale_first = lax.rsqrt(square / model_width + EPS)
        tail = tail * scale_first
        query, key, value, outgate = (
            (scale_first * summed[own_seqs * i + s : own_seqs * i + s + 1, :own_width])
            .astype(bf16)
            .astype(f32)
            for i in range(4)
        )
        query = query * inv_root
        hidden_parts = []
        for h in range(head_count):
            cols = slice(h * head_size, (h + 1) * head_size)
            in_gate = tail[:, h : h + 1]
            forget_arg = tail[:, head_count + h : head_count + h + 1]
            forget_new = jnp.minimum(forget_arg, 0.0) - jnp.log1p(jnp.exp(-jnp.abs(forget_arg)))
            state_log = base_total[s, h] + forget_new + sx_v[s : s + 1, h : h + 1]
            peak_log = jnp.maximum(
                jnp.maximum(state_log, in_gate), base_max[s, h] + forget_new
            )
            q = query[:, cols]
            q_low = q.astype(bf16)
            dots = lax.dot_general(
                q_low, ck_v[s, :, cols], contract_last, preferred_element_type=f32
            )
            scores = jnp.exp(base_log[s, h] + forget_new - peak_log) * dots
            self_score = jnp.exp(in_gate - peak_log) * jnp.sum(
                q * key[:, cols], axis=1, keepdims=True
            )
            carried = jnp.exp(state_log - peak_log)
            read = lax.dot_general(
                q_low, hi_v[s, h], contract_last, preferred_element_type=f32
            ) + lax.dot_general(q_low, lo_v[s, h], contract_last, preferred_element_type=f32)
            norm_read = jnp.sum(sn_v[s, h : h + 1, :] * q, axis=1, keepdims=True)
            numerator = (
                carried * read
                + jnp.dot(scores.astype(bf16), cv_v[s, :, cols], preferred_element_type=f32)
                + self_score * value[:, cols]
            )
            denominator = (
                carried * norm_read + jnp.sum(scores, axis=1, keepdims=True) + self_score
            )
            hidden = numerator / jnp.maximum(jnp.abs(denominator), 1.0)
            hidden_parts.append(hidden * hg_v[:, cols] * jax.nn.sigmoid(outgate[:, cols]))
        mixed_rows.append(jnp.concatenate(hidden_parts, axis=1))
    for s in range(own_seqs):
        mixed_all[me, s : s + 1, :] = mixed_rows[s].astype(bf16).astype(f32)
    mixed_copies = {}
    for d in kv_far:
        mixed_copies[d] = remote(
            mixed_all.at[me],
            mixed_all.at[me],
            mixed_ssem.at[d - 1],
            mixed_rsem.at[lax.rem(me + 0, kv_count)],
            d,
            0,
        )
        mixed_copies[d].start()
    loads[17].wait()
    for d in range(1, kv_count):
        source = lax.rem(me + kv_count - d, kv_count)
        remote(
            mixed_all.at[source], mixed_all.at[source], mixed_ssem.at[d - 1],
            mixed_rsem.at[source], d, 0,
        ).wait_recv()
    mixed = jnp.concatenate([mixed_all[r] for r in range(kv_count)], axis=0).astype(bf16)
    own_half = jnp.dot(mixed, outw_v[...], preferred_element_type=f32).astype(bf16)
    half_send[...] = own_half
    half_copies = {}
    for i in far_first:
        dk, dt = peers[i]
        half_copies[i] = remote(
            half_send, half_recv.at[i], half_ssem.at[i], half_rsem.at[i], dk, dt
        )
        half_copies[i].start()
    for i in range(18, 21):
        loads[i].wait()
    sum_squares = jnp.zeros((rows, 1), f32)
    gate_acc = jnp.zeros((rows, gw_v.shape[0]), f32)
    up_acc = jnp.zeros((rows, gw_v.shape[0]), f32)
    own_residual = None
    for dk in sorted(range(kv_count), key=lambda d: min(d, kv_count - d)):
        source = lax.rem(me + kv_count - dk, kv_count)
        halves = [own_half.astype(f32)] if dk == 0 else []
        for i, (pk, pt) in enumerate(peers):
            if pk == dk:
                half_copies[i].wait_recv()
                halves.append(half_recv[i].astype(f32))
        if dk:
            tok_copies[dk].wait_recv()
            chunk_tokens = tok_recv[dk - 1].astype(f32)
        else:
            chunk_tokens = token_values
        residual = (chunk_tokens + sum(halves[1:], halves[0])).astype(bf16).astype(f32)
        if dk == 0:
            own_residual = residual
        sum_squares = sum_squares + jnp.sum(residual * residual, axis=1, keepdims=True)
        at = pl.multiple_of(source * width, 128)
        normed_mid = (residual * mg_v[:, pl.ds(at, width)]).astype(bf16)
        gate_acc = gate_acc + lax.dot_general(
            normed_mid, gw_v[:, pl.ds(at, width)], contract_last, preferred_element_type=f32
        )
        up_acc = up_acc + lax.dot_general(
            normed_mid, uw_v[:, pl.ds(at, width)], contract_last, preferred_element_type=f32
        )
    scale_mid = lax.rsqrt(sum_squares / model_width + EPS)
    hidden_units = (jax.nn.silu(scale_mid * gate_acc) * (scale_mid * up_acc)).astype(bf16)
    loads[21].wait()

    def down_part(dk, dt):
        target = lax.rem(me + dk, kv_count) * tp_count + lax.rem(core + dt, tp_count)
        at = pl.multiple_of(target * narrow, 128)
        return jnp.dot(hidden_units, dw_v[:, pl.ds(at, narrow)], preferred_element_type=f32)

    down_copies = {}
    for i in far_first:
        dk, dt = peers[i]
        down_send[i] = down_part(dk, dt).astype(down_send.dtype)
        down_copies[i] = remote(
            down_send.at[i], down_recv.at[i], down_ssem.at[i], down_rsem.at[i], dk, dt
        )
        down_copies[i].start()
    total_out = own_residual[:, :narrow]
    for t in range(1, tp_count):
        total_out = jnp.where(
            core == t, own_residual[:, t * narrow : (t + 1) * narrow], total_out
        )
    mixer_out = down_part(0, 0)
    for i in near_first:
        down_copies[i].wait_recv()
        mixer_out = mixer_out + down_recv[i].astype(f32)
    out[...] = (total_out + mixer_out).astype(out.dtype)

    for copies in (proj_copies, tok_copies, mixed_copies, half_copies, down_copies):
        for copy in copies.values():
            copy.wait_send()


def fused_device(mesh, *args):
    (tokens, pre_gain, query_weight, _, _, _, input_gate_weight, forget_gate_weight) = args[:8]
    cache_keys, cache_values, cache_input, cache_forget, lengths = args[8:13]
    state_matrix, state_norm, state_max, head_gain, out_weight = args[13:18]
    mixer_gain, gate_weight, up_weight, down_weight = args[18:]
    kv_count, tp_count = mesh.shape["kv"], mesh.shape["tp"]
    f32, bf16 = jnp.float32, jnp.bfloat16
    rows, width = tokens.shape
    own_seqs = cache_keys.shape[0]
    own_width = query_weight.shape[1]
    narrow = width // tp_count
    peer_count = kv_count * tp_count - 1
    given = list(args)
    given[1] = pre_gain[None, :]
    given[6] = input_gate_weight.T
    given[7] = forget_gate_weight.T
    given[12] = lengths[None, :]
    given[10] = jnp.swapaxes(cache_input, 1, 2)
    given[11] = jnp.swapaxes(cache_forget, 1, 2)
    given[16] = head_gain[None, :]
    given[18] = mixer_gain[None, :]
    given[19] = gate_weight.T
    given[20] = up_weight.T

    def held(array):
        return pltpu.VMEM(array.shape, array.dtype)

    gate_heads = input_gate_weight.shape[1]
    dma = pltpu.SemaphoreType.DMA
    scratch = [
        held(tokens),
        held(given[1]),
        pltpu.VMEM((4,) + query_weight.shape, bf16),
        pltpu.VMEM((gate_heads, width), bf16),
        pltpu.VMEM((gate_heads, width), bf16),
        held(cache_keys),
        held(cache_values),
        held(given[10]),
        held(given[11]),
        held(given[12]),
        held(state_matrix),
        held(state_norm),
        held(state_max),
        held(given[16]),
        held(out_weight),
        held(given[18]),
        held(given[19]),
        held(given[20]),
        held(down_weight),
        pltpu.VMEM(state_matrix.shape, bf16),
        pltpu.VMEM(state_matrix.shape, bf16),
        pltpu.VMEM((kv_count, 4 * own_seqs, own_width + 128), f32),
        pltpu.VMEM((kv_count - 1, 4 * own_seqs, own_width + 128), f32),
        pltpu.VMEM((kv_count - 1, rows, width), bf16),
        pltpu.VMEM((kv_count, own_seqs, own_width), f32),
        pltpu.VMEM((rows, width), bf16),
        pltpu.VMEM((peer_count, rows, width), bf16),
        pltpu.VMEM((peer_count, rows, narrow), bf16),
        pltpu.VMEM((peer_count, rows, narrow), bf16),
        dma((len(args),)),
        dma((kv_count - 1,)),
        dma((kv_count - 1,)),
        dma((kv_count - 1,)),
        dma((kv_count - 1,)),
        dma((kv_count - 1,)),
        dma((kv_count,)),
        dma((peer_count,)),
        dma((peer_count,)),
        dma((peer_count,)),
        dma((peer_count,)),
    ]
    return pl.pallas_call(
        functools.partial(cell_kernel, kv_count, tp_count),
        out_shape=jax.ShapeDtypeStruct((rows, narrow), tokens.dtype),
        in_specs=[pl.BlockSpec(memory_space=pl.ANY)] * len(args),
        out_specs=pl.BlockSpec(memory_space=pltpu.VMEM),
        scratch_shapes=scratch,
        compiler_params=pltpu.CompilerParams(
            collective_id=0, has_side_effects=True, vmem_limit_bytes=60 * 1024 * 1024
        ),
    )(*given)


def fits_tiles(mesh, tokens, query_weight, cache_keys, state_norm):
    kv_count, tp_count = mesh.shape["kv"], mesh.shape["tp"]
    return (
        tokens.shape[1] % (kv_count * tp_count * 128) == 0
        and query_weight.shape[1] % (tp_count * 128) == 0
        and state_norm.shape[2] % 128 == 0
        and kv_count > 1
    )


def solution(mesh):
    in_specs = (
        P("dp", "kv"),
        P("kv"),
        P("kv", "tp"),
        P("kv", "tp"),
        P("kv", "tp"),
        P("kv", "tp"),
        P(),
        P(),
        P(("dp", "kv"), None, "tp"),
        P(("dp", "kv"), None, "tp"),
        P(("dp", "kv"), None, "tp"),
        P(("dp", "kv"), None, "tp"),
        P(("dp", "kv")),
        P(("dp", "kv"), "tp", None, None),
        P(("dp", "kv"), "tp", None),
        P(("dp", "kv"), "tp"),
        P("tp"),
        P("tp", "kv"),
        P(),
        P(None, ("kv", "tp")),
        P(None, ("kv", "tp")),
        P(("kv", "tp"), None),
    )
    out_specs = P("dp", ("kv", "tp"))

    def run(*args):
        fused = fits_tiles(mesh, args[0], args[2], args[8], args[14])
        body = functools.partial(fused_device, mesh) if fused else per_device
        return jax.shard_map(
            body, mesh=mesh, in_specs=in_specs, out_specs=out_specs, check_vma=False
        )(*args)

    return run
```

```python
import functools

import jax
import jax.numpy as jnp
from jax import lax
from jax.experimental import pallas as pl
from jax.experimental.pallas import tpu as pltpu
from jax.sharding import PartitionSpec as P

EPS = 1e-06


def per_device(
    tokens,
    pre_gain,
    query_weight,
    key_weight,
    value_weight,
    outgate_weight,
    input_gate_weight,
    forget_gate_weight,
    cache_keys,
    cache_values,
    cache_input,
    cache_forget,
    lengths,
    state_matrix,
    state_norm,
    state_max,
    head_gain,
    out_weight,
    mixer_gain,
    gate_weight,
    up_weight,
    down_weight,
):
    col_width = tokens.shape[1]
    own_seqs = cache_keys.shape[0]
    block_len = cache_keys.shape[1]
    head_count = state_max.shape[1]
    head_size = state_norm.shape[2]
    shard_index = lax.axis_index("kv")
    half_index = lax.axis_index("tp")
    kv_count = lax.axis_size("kv")
    model_width = col_width * kv_count
    token_values = tokens.astype(jnp.float32)
    squares = jnp.sum(token_values * token_values, axis=1)
    normed = (token_values * pre_gain[None, :]).astype(jnp.bfloat16)
    corner = (shard_index * col_width, half_index * head_count)
    gate_pair = jnp.concatenate(
        [
            lax.dynamic_slice(input_gate_weight, corner, (col_width, head_count)),
            lax.dynamic_slice(forget_gate_weight, corner, (col_width, head_count)),
        ],
        axis=1,
    )

    def product(weight):
        return jnp.dot(normed, weight, preferred_element_type=jnp.float32)

    query_term = product(query_weight)
    key_term = product(key_weight)
    value_term = product(value_weight)
    outgate_term = product(outgate_weight)
    gate_term = product(gate_pair)
    square_totals = lax.psum(squares, "kv")
    query_sum, key_sum, value_sum, outgate_sum, gate_sum = (
        lax.psum_scatter(query_term, "kv", scatter_dimension=0, tiled=True),
        lax.psum_scatter(key_term, "kv", scatter_dimension=0, tiled=True),
        lax.psum_scatter(value_term, "kv", scatter_dimension=0, tiled=True),
        lax.psum_scatter(outgate_term, "kv", scatter_dimension=0, tiled=True),
        lax.psum_scatter(gate_term, "kv", scatter_dimension=0, tiled=True),
    )
    own_squares = lax.dynamic_slice_in_dim(square_totals, shard_index * own_seqs, own_seqs, 0)
    scale_first = lax.rsqrt(own_squares / model_width + EPS)[:, None]
    query = (scale_first * query_sum).astype(jnp.bfloat16)
    keys_new = (scale_first * key_sum).astype(jnp.bfloat16)
    values_new = (scale_first * value_sum).astype(jnp.bfloat16)
    outgate = (scale_first * outgate_sum).astype(jnp.bfloat16)
    gate_values = scale_first * gate_sum
    in_gate = gate_values[:, :head_count]
    forget_new = jax.nn.log_sigmoid(gate_values[:, head_count:])
    query_heads = query.reshape(own_seqs, head_count, head_size)
    key_heads = keys_new.reshape(own_seqs, head_count, head_size)
    value_heads = values_new.reshape(own_seqs, head_count, head_size)
    cached_keys = cache_keys.reshape(own_seqs, block_len, head_count, head_size)
    cached_values = cache_values.reshape(own_seqs, block_len, head_count, head_size)
    inv_root = head_size ** (-0.5)
    live_mask = (lax.broadcasted_iota(jnp.int32, (own_seqs, block_len), 1) < lengths[:, None])[
        :, :, None
    ]
    forget_live = jnp.where(live_mask, cache_forget, jnp.float32(0.0))
    running = jnp.cumsum(forget_live, axis=1)
    total_log = running[:, -1, :] + forget_new
    weight_log = jnp.where(live_mask, total_log[:, None, :] - running + cache_input, -jnp.inf)
    state_log = total_log + state_max
    peak_log = jnp.maximum(jnp.maximum(state_log, in_gate), jnp.max(weight_log, axis=1))
    key_dots = (
        jnp.einsum("shd,slhd->slh", query_heads, cached_keys, preferred_element_type=jnp.float32)
        * inv_root
    )
    block_scores = jnp.exp(weight_log - peak_log[:, None, :]) * key_dots
    query_scaled = query_heads.astype(jnp.float32) * inv_root
    self_score = jnp.exp(in_gate - peak_log) * jnp.sum(
        query_scaled * key_heads.astype(jnp.float32), axis=2
    )
    carried = jnp.exp(state_log - peak_log)
    block_weights = block_scores.astype(jnp.bfloat16)
    memory_read = jnp.einsum(
        "shvd,shd->shv", state_matrix, query_scaled, precision=lax.Precision.HIGHEST
    )
    norm_read = jnp.einsum("shd,shd->sh", state_norm, query_scaled, precision=lax.Precision.HIGHEST)
    numerator = (
        carried[:, :, None] * memory_read
        + jnp.einsum(
            "slh,slhd->shd", block_weights, cached_values, preferred_element_type=jnp.float32
        )
        + self_score[:, :, None] * value_heads.astype(jnp.float32)
    )
    denominator = carried * norm_read + jnp.sum(block_scores, axis=1) + self_score
    hidden = numerator / jnp.maximum(jnp.abs(denominator), 1.0)[:, :, None]
    mixed_heads = (
        hidden.reshape(own_seqs, head_count * head_size)
        * head_gain[None, :]
        * jax.nn.sigmoid(outgate.astype(jnp.float32))
    ).astype(jnp.bfloat16)
    mix_terms = jnp.dot(
        lax.all_gather(mixed_heads, "kv", axis=0, tiled=True),
        out_weight,
        preferred_element_type=jnp.float32,
    )
    mix_sum = lax.psum_scatter(
        mix_terms.astype(jnp.bfloat16), "tp", scatter_dimension=1, tiled=True
    ).astype(jnp.float32)
    narrow = mix_sum.shape[1]
    residual = (
        lax.dynamic_slice_in_dim(token_values, half_index * narrow, narrow, 1) + mix_sum
    ).astype(jnp.bfloat16)
    piece_wide = lax.all_gather(residual, ("kv", "tp"), axis=1, tiled=True).astype(jnp.float32)
    normed_piece = (piece_wide * mixer_gain[None, :]).astype(jnp.bfloat16)
    gate_acc = jnp.dot(normed_piece, gate_weight, preferred_element_type=jnp.float32)
    up_acc = jnp.dot(normed_piece, up_weight, preferred_element_type=jnp.float32)
    sum_squares = jnp.sum(piece_wide * piece_wide, axis=1)
    gate_acc, up_acc, sum_squares = (gate_acc, up_acc, sum_squares)
    scale_mid = lax.rsqrt(sum_squares / model_width + EPS)[:, None]
    hidden_units = (jax.nn.silu(scale_mid * gate_acc) * (scale_mid * up_acc)).astype(jnp.bfloat16)
    summed = lax.psum_scatter(
        lax.dot_general(
            down_weight, hidden_units, (((0,), (1,)), ((), ())), preferred_element_type=jnp.float32
        ),
        ("kv", "tp"),
        scatter_dimension=0,
        tiled=True,
    )
    mixer_out = summed.T
    return (residual.astype(jnp.float32) + mixer_out).astype(jnp.bfloat16)


def cell_kernel(
    kv_count,
    tp_count,
    tokens,
    pre_gain,
    query_weight,
    key_weight,
    value_weight,
    outgate_weight,
    input_gate_weight,
    forget_gate_weight,
    cache_keys,
    cache_values,
    cache_input,
    cache_forget,
    lengths,
    state_matrix,
    state_norm,
    state_max,
    head_gain,
    out_weight,
    mixer_gain,
    gate_weight,
    up_weight,
    down_weight,
    out,
    tok_v,
    pg_v,
    proj_v,
    igw_v,
    fgw_v,
    ck_v,
    cv_v,
    ci_v,
    cf_v,
    len_v,
    sm_v,
    sn_v,
    sx_v,
    hg_v,
    outw_v,
    mg_v,
    gw_v,
    uw_v,
    dw_v,
    hi_v,
    lo_v,
    proj_send,
    proj_recv,
    proj_own,
    small_send,
    small_recv,
    tok_recv,
    mixed_all,
    half_send,
    half_recv,
    down_send,
    down_recv,
    local_sem,
    proj_ssem,
    proj_rsem,
    small_ssem,
    small_rsem,
    tok_ssem,
    tok_rsem,
    mixed_ssem,
    mixed_rsem,
    half_ssem,
    half_rsem,
    down_ssem,
    down_rsem,
):
    f32, bf16 = jnp.float32, jnp.bfloat16
    me = lax.axis_index("kv")
    core = lax.axis_index("tp")
    rows, width = tok_v.shape
    own_seqs, block_len = ck_v.shape[0], ck_v.shape[1]
    head_count, head_size = sn_v.shape[1], sn_v.shape[2]
    own_width = head_count * head_size
    model_width = width * kv_count
    narrow = out.shape[1]
    peers = [(dk, dt) for dk in range(kv_count) for dt in range(tp_count) if dk or dt]
    far_first = sorted(range(len(peers)), key=lambda i: -min(peers[i][0], kv_count - peers[i][0]))
    near_first = far_first[::-1]
    kv_far = sorted(range(1, kv_count), key=lambda d: -min(d, kv_count - d))

    def peer(dk, dt):
        return {"kv": lax.rem(me + dk, kv_count), "tp": lax.rem(core + dt, tp_count)}

    sources = (
        (tokens, tok_v),
        (pre_gain, pg_v),
        (query_weight, proj_v.at[0]),
        (key_weight, proj_v.at[1]),
        (value_weight, proj_v.at[2]),
        (outgate_weight, proj_v.at[3]),
        (input_gate_weight.at[:, pl.ds(pl.multiple_of(me * width, 128), width)], igw_v),
        (forget_gate_weight.at[:, pl.ds(pl.multiple_of(me * width, 128), width)], fgw_v),
        (cache_forget, cf_v),
        (cache_input, ci_v),
        (lengths, len_v),
        (state_max, sx_v),
        (state_norm, sn_v),
        (head_gain, hg_v),
        (state_matrix, sm_v),
        (cache_keys, ck_v),
        (cache_values, cv_v),
        (out_weight, outw_v),
        (mixer_gain, mg_v),
        (gate_weight, gw_v),
        (up_weight, uw_v),
        (down_weight, dw_v),
    )
    loads = [
        pltpu.make_async_copy(src, dst, local_sem.at[i]) for i, (src, dst) in enumerate(sources)
    ]
    for load in loads[:8]:
        load.start()

    barrier = pltpu.get_barrier_semaphore()
    for dk, dt in peers:
        pl.semaphore_signal(
            barrier, inc=1, device_id=peer(dk, dt), device_id_type=pl.DeviceIdType.MESH
        )

    def remote(src, dst, ssem, rsem, dk, dt):
        return pltpu.make_async_remote_copy(
            src_ref=src,
            dst_ref=dst,
            send_sem=ssem,
            recv_sem=rsem,
            device_id=peer(dk, dt),
            device_id_type=pl.DeviceIdType.MESH,
        )

    for i in range(2):
        loads[i].wait()
    token_values = tok_v[...].astype(f32)
    squares = jnp.sum(token_values * token_values, axis=1, keepdims=True)
    normed = (token_values * pg_v[...]).astype(bf16)
    terms = []
    for i in range(4):
        loads[2 + i].wait()
        terms.append(jnp.dot(normed, proj_v[i], preferred_element_type=f32))
    for r in range(kv_count):
        block = jnp.concatenate(
            [term[own_seqs * r : own_seqs * (r + 1), :] for term in terms], axis=0
        )
        proj_send[r] = block.astype(proj_send.dtype)
        proj_own[r] = block
    loads[6].wait()
    loads[7].wait()
    for load in loads[8:]:
        load.start()
    contract_last = (((1,), (1,)), ((), ()))
    gates = [
        lax.dot_general(normed, ref[...], contract_last, preferred_element_type=f32)
        for ref in (igw_v, fgw_v)
    ]
    lane = lax.broadcasted_iota(jnp.int32, (rows, 128), 1)
    small = jnp.where(lane == 2 * head_count, squares, 0.0)
    for g in range(2):
        for h in range(head_count):
            column = gates[g][:, h : h + 1]
            for t in range(1, tp_count):
                at = t * head_count + h
                column = jnp.where(core == t, gates[g][:, at : at + 1], column)
            small = jnp.where(lane == g * head_count + h, column, small)
    for r in range(kv_count):
        small_send[r] = jnp.concatenate([small[own_seqs * r : own_seqs * (r + 1), :]] * 4, axis=0)

    pl.semaphore_wait(barrier, len(peers))
    proj_copies = {}
    for d in kv_far:
        proj_copies[d] = remote(
            proj_send.at[lax.rem(me + d, kv_count)],
            proj_recv.at[d - 1],
            proj_ssem.at[d - 1],
            proj_rsem.at[d - 1],
            d,
            0,
        )
        proj_copies[d].start()
    small_copies = {}
    for d in kv_far:
        small_copies[d] = remote(
            small_send.at[lax.rem(me + d, kv_count)],
            small_recv.at[d - 1],
            small_ssem.at[d - 1],
            small_rsem.at[d - 1],
            d,
            0,
        )
        small_copies[d].start()
    tok_copies = {}
    for d in kv_far:
        tok_copies[d] = remote(
            tok_v, tok_recv.at[d - 1], tok_ssem.at[d - 1], tok_rsem.at[d - 1], d, 0
        )
        tok_copies[d].start()

    for i in range(8, 15):
        loads[i].wait()
    for s in range(own_seqs):
        for h in range(head_count):
            whole = sm_v[s, h]
            high = whole.astype(bf16)
            hi_v[s, h] = high
            lo_v[s, h] = (whole - high.astype(f32)).astype(bf16)
    at_row = lax.broadcasted_iota(jnp.int32, (block_len, block_len), 0)
    at_col = lax.broadcasted_iota(jnp.int32, (block_len, block_len), 1)
    position_row = lax.broadcasted_iota(jnp.int32, (1, block_len), 1)
    up_to = (at_row <= at_col).astype(f32)
    base_log, base_max, base_total = {}, {}, {}
    for s in range(own_seqs):
        live = position_row < len_v[0:1, s : s + 1]
        running_all = jnp.dot(
            jnp.where(live, cf_v[s], 0.0),
            up_to,
            precision=lax.Precision.HIGHEST,
            preferred_element_type=f32,
        )
        for h in range(head_count):
            running = running_all[h : h + 1, :]
            total = running[:, block_len - 1 : block_len]
            logs = jnp.where(live, total - running + ci_v[s, h : h + 1, :], -jnp.inf)
            base_log[s, h] = logs
            base_max[s, h] = jnp.max(logs, axis=1, keepdims=True)
            base_total[s, h] = total
    for i in range(15, 17):
        loads[i].wait()

    summed = proj_own[me]
    tails = small_send[me]
    for d in range(1, kv_count):
        proj_copies[d].wait_recv()
        summed = summed + proj_recv[d - 1].astype(f32)
        small_copies[d].wait_recv()
        tails = tails + small_recv[d - 1]
    inv_root = head_size ** (-0.5)
    mixed_rows = []
    for s in range(own_seqs):
        tail = tails[s : s + 1, :]
        square = tail[:, 2 * head_count : 2 * head_count + 1]
        scale_first = lax.rsqrt(square / model_width + EPS)
        tail = tail * scale_first
        query, key, value, outgate = (
            (scale_first * summed[own_seqs * i + s : own_seqs * i + s + 1, :])
            .astype(bf16)
            .astype(f32)
            for i in range(4)
        )
        query = query * inv_root
        hidden_parts = []
        for h in range(head_count):
            cols = slice(h * head_size, (h + 1) * head_size)
            in_gate = tail[:, h : h + 1]
            forget_arg = tail[:, head_count + h : head_count + h + 1]
            forget_new = jnp.minimum(forget_arg, 0.0) - jnp.log1p(jnp.exp(-jnp.abs(forget_arg)))
            state_log = base_total[s, h] + forget_new + sx_v[s : s + 1, h : h + 1]
            peak_log = jnp.maximum(
                jnp.maximum(state_log, in_gate), base_max[s, h] + forget_new
            )
            q = query[:, cols]
            q_low = q.astype(bf16)
            dots = lax.dot_general(
                q_low, ck_v[s, :, cols], contract_last, preferred_element_type=f32
            )
            scores = jnp.exp(base_log[s, h] + forget_new - peak_log) * dots
            self_score = jnp.exp(in_gate - peak_log) * jnp.sum(
                q * key[:, cols], axis=1, keepdims=True
            )
            carried = jnp.exp(state_log - peak_log)
            read = lax.dot_general(
                q_low, hi_v[s, h], contract_last, preferred_element_type=f32
            ) + lax.dot_general(q_low, lo_v[s, h], contract_last, preferred_element_type=f32)
            norm_read = jnp.sum(sn_v[s, h : h + 1, :] * q, axis=1, keepdims=True)
            numerator = (
                carried * read
                + jnp.dot(scores.astype(bf16), cv_v[s, :, cols], preferred_element_type=f32)
                + self_score * value[:, cols]
            )
            denominator = (
                carried * norm_read + jnp.sum(scores, axis=1, keepdims=True) + self_score
            )
            hidden = numerator / jnp.maximum(jnp.abs(denominator), 1.0)
            hidden_parts.append(hidden * hg_v[:, cols] * jax.nn.sigmoid(outgate[:, cols]))
        mixed_rows.append(jnp.concatenate(hidden_parts, axis=1))
    for s in range(own_seqs):
        mixed_all[me, s : s + 1, :] = mixed_rows[s].astype(bf16).astype(f32)
    mixed_copies = {}
    for d in kv_far:
        mixed_copies[d] = remote(
            mixed_all.at[me],
            mixed_all.at[me],
            mixed_ssem.at[d - 1],
            mixed_rsem.at[lax.rem(me + 0, kv_count)],
            d,
            0,
        )
        mixed_copies[d].start()
    loads[17].wait()
    for d in range(1, kv_count):
        source = lax.rem(me + kv_count - d, kv_count)
        remote(
            mixed_all.at[source], mixed_all.at[source], mixed_ssem.at[d - 1],
            mixed_rsem.at[source], d, 0,
        ).wait_recv()
    mixed = jnp.concatenate([mixed_all[r] for r in range(kv_count)], axis=0).astype(bf16)
    own_half = jnp.dot(mixed, outw_v[...], preferred_element_type=f32).astype(bf16)
    half_send[...] = own_half
    half_copies = {}
    for i in far_first:
        dk, dt = peers[i]
        half_copies[i] = remote(
            half_send, half_recv.at[i], half_ssem.at[i], half_rsem.at[i], dk, dt
        )
        half_copies[i].start()
    for i in range(18, 21):
        loads[i].wait()
    sum_squares = jnp.zeros((rows, 1), f32)
    gate_acc = jnp.zeros((rows, gw_v.shape[0]), f32)
    up_acc = jnp.zeros((rows, gw_v.shape[0]), f32)
    own_residual = None
    for dk in sorted(range(kv_count), key=lambda d: min(d, kv_count - d)):
        source = lax.rem(me + kv_count - dk, kv_count)
        halves = [own_half.astype(f32)] if dk == 0 else []
        for i, (pk, pt) in enumerate(peers):
            if pk == dk:
                half_copies[i].wait_recv()
                halves.append(half_recv[i].astype(f32))
        if dk:
            tok_copies[dk].wait_recv()
            chunk_tokens = tok_recv[dk - 1].astype(f32)
        else:
            chunk_tokens = token_values
        residual = (chunk_tokens + sum(halves[1:], halves[0])).astype(bf16).astype(f32)
        if dk == 0:
            own_residual = residual
        sum_squares = sum_squares + jnp.sum(residual * residual, axis=1, keepdims=True)
        at = pl.multiple_of(source * width, 128)
        normed_mid = (residual * mg_v[:, pl.ds(at, width)]).astype(bf16)
        gate_acc = gate_acc + lax.dot_general(
            normed_mid, gw_v[:, pl.ds(at, width)], contract_last, preferred_element_type=f32
        )
        up_acc = up_acc + lax.dot_general(
            normed_mid, uw_v[:, pl.ds(at, width)], contract_last, preferred_element_type=f32
        )
    scale_mid = lax.rsqrt(sum_squares / model_width + EPS)
    hidden_units = (jax.nn.silu(scale_mid * gate_acc) * (scale_mid * up_acc)).astype(bf16)
    loads[21].wait()

    def down_part(dk, dt):
        target = lax.rem(me + dk, kv_count) * tp_count + lax.rem(core + dt, tp_count)
        at = pl.multiple_of(target * narrow, 128)
        return jnp.dot(hidden_units, dw_v[:, pl.ds(at, narrow)], preferred_element_type=f32)

    down_copies = {}
    for i in far_first:
        dk, dt = peers[i]
        down_send[i] = down_part(dk, dt).astype(down_send.dtype)
        down_copies[i] = remote(
            down_send.at[i], down_recv.at[i], down_ssem.at[i], down_rsem.at[i], dk, dt
        )
        down_copies[i].start()
    total_out = own_residual[:, :narrow]
    for t in range(1, tp_count):
        total_out = jnp.where(
            core == t, own_residual[:, t * narrow : (t + 1) * narrow], total_out
        )
    mixer_out = down_part(0, 0)
    for i in near_first:
        down_copies[i].wait_recv()
        mixer_out = mixer_out + down_recv[i].astype(f32)
    out[...] = (total_out + mixer_out).astype(out.dtype)

    for copies in (proj_copies, small_copies, tok_copies, mixed_copies, half_copies, down_copies):
        for copy in copies.values():
            copy.wait_send()


def fused_device(mesh, *args):
    (tokens, pre_gain, query_weight, _, _, _, input_gate_weight, forget_gate_weight) = args[:8]
    cache_keys, cache_values, cache_input, cache_forget, lengths = args[8:13]
    state_matrix, state_norm, state_max, head_gain, out_weight = args[13:18]
    mixer_gain, gate_weight, up_weight, down_weight = args[18:]
    kv_count, tp_count = mesh.shape["kv"], mesh.shape["tp"]
    f32, bf16 = jnp.float32, jnp.bfloat16
    rows, width = tokens.shape
    own_seqs = cache_keys.shape[0]
    own_width = query_weight.shape[1]
    narrow = width // tp_count
    peer_count = kv_count * tp_count - 1
    given = list(args)
    given[1] = pre_gain[None, :]
    given[6] = input_gate_weight.T
    given[7] = forget_gate_weight.T
    given[12] = lengths[None, :]
    given[10] = jnp.swapaxes(cache_input, 1, 2)
    given[11] = jnp.swapaxes(cache_forget, 1, 2)
    given[16] = head_gain[None, :]
    given[18] = mixer_gain[None, :]
    given[19] = gate_weight.T
    given[20] = up_weight.T

    def held(array):
        return pltpu.VMEM(array.shape, array.dtype)

    gate_heads = input_gate_weight.shape[1]
    dma = pltpu.SemaphoreType.DMA
    scratch = [
        held(tokens),
        held(given[1]),
        pltpu.VMEM((4,) + query_weight.shape, bf16),
        pltpu.VMEM((gate_heads, width), bf16),
        pltpu.VMEM((gate_heads, width), bf16),
        held(cache_keys),
        held(cache_values),
        held(given[10]),
        held(given[11]),
        held(given[12]),
        held(state_matrix),
        held(state_norm),
        held(state_max),
        held(given[16]),
        held(out_weight),
        held(given[18]),
        held(given[19]),
        held(given[20]),
        held(down_weight),
        pltpu.VMEM(state_matrix.shape, bf16),
        pltpu.VMEM(state_matrix.shape, bf16),
        pltpu.VMEM((kv_count, 4 * own_seqs, own_width), bf16),
        pltpu.VMEM((kv_count - 1, 4 * own_seqs, own_width), bf16),
        pltpu.VMEM((kv_count, 4 * own_seqs, own_width), f32),
        pltpu.VMEM((kv_count, 4 * own_seqs, 128), f32),
        pltpu.VMEM((kv_count - 1, 4 * own_seqs, 128), f32),
        pltpu.VMEM((kv_count - 1, rows, width), bf16),
        pltpu.VMEM((kv_count, own_seqs, own_width), f32),
        pltpu.VMEM((rows, width), bf16),
        pltpu.VMEM((peer_count, rows, width), bf16),
        pltpu.VMEM((peer_count, rows, narrow), bf16),
        pltpu.VMEM((peer_count, rows, narrow), bf16),
        dma((len(args),)),
        dma((kv_count - 1,)),
        dma((kv_count - 1,)),
        dma((kv_count - 1,)),
        dma((kv_count - 1,)),
        dma((kv_count - 1,)),
        dma((kv_count - 1,)),
        dma((kv_count - 1,)),
        dma((kv_count,)),
        dma((peer_count,)),
        dma((peer_count,)),
        dma((peer_count,)),
        dma((peer_count,)),
    ]
    return pl.pallas_call(
        functools.partial(cell_kernel, kv_count, tp_count),
        out_shape=jax.ShapeDtypeStruct((rows, narrow), tokens.dtype),
        in_specs=[pl.BlockSpec(memory_space=pl.ANY)] * len(args),
        out_specs=pl.BlockSpec(memory_space=pltpu.VMEM),
        scratch_shapes=scratch,
        compiler_params=pltpu.CompilerParams(
            collective_id=0, has_side_effects=True, vmem_limit_bytes=60 * 1024 * 1024
        ),
    )(*given)


def fits_tiles(mesh, tokens, query_weight, cache_keys, state_norm):
    kv_count, tp_count = mesh.shape["kv"], mesh.shape["tp"]
    return (
        tokens.shape[1] % (kv_count * tp_count * 128) == 0
        and query_weight.shape[1] % (tp_count * 128) == 0
        and state_norm.shape[2] % 128 == 0
        and kv_count > 1
    )


def solution(mesh):
    in_specs = (
        P("dp", "kv"),
        P("kv"),
        P("kv", "tp"),
        P("kv", "tp"),
        P("kv", "tp"),
        P("kv", "tp"),
        P(),
        P(),
        P(("dp", "kv"), None, "tp"),
        P(("dp", "kv"), None, "tp"),
        P(("dp", "kv"), None, "tp"),
        P(("dp", "kv"), None, "tp"),
        P(("dp", "kv")),
        P(("dp", "kv"), "tp", None, None),
        P(("dp", "kv"), "tp", None),
        P(("dp", "kv"), "tp"),
        P("tp"),
        P("tp", "kv"),
        P(),
        P(None, ("kv", "tp")),
        P(None, ("kv", "tp")),
        P(("kv", "tp"), None),
    )
    out_specs = P("dp", ("kv", "tp"))

    def run(*args):
        fused = fits_tiles(mesh, args[0], args[2], args[8], args[14])
        body = functools.partial(fused_device, mesh) if fused else per_device
        return jax.shard_map(
            body, mesh=mesh, in_specs=in_specs, out_specs=out_specs, check_vma=False
        )(*args)

    return run
```
